512 devices in a mesh: rep: 16 (over z), fs: 4 (over y), tp: 8 (over x, core).
Axes of the slice: x: 4, y: 4, z: 16, core: 2. Of those that a mesh axis runs over, the one named last changes fastest.
Arguments:
- inputs: bfloat16 [8192, 2048], P('rep', 'fs'), may hold values from -6 to 6
- w_gate: bfloat16 [2048, 3072], P('fs', 'tp'), may hold values from -0.125 to 0.125
- w_up: bfloat16 [2048, 3072], P('fs', 'tp'), may hold values from -0.125 to 0.125
- conv_taps: bfloat16 [3, 3072], P(None, 'tp'), may hold values from -3.5 to 3.5
- w_down: bfloat16 [3072, 2048], P('tp', 'fs'), may hold values from -0.109375 to 0.109375
- out_grad: bfloat16 [8192, 2048], P('rep', 'fs'), may hold values from -6 to 6
Outputs:
- in_grad: bfloat16 [8192, 2048], P(('rep', 'tp'), 'fs')
- grad_gate: float32 [2048, 3072], P('fs', 'tp')
- grad_up: float32 [2048, 3072], P('fs', 'tp')
- grad_down: float32 [3072, 2048], P('tp', 'fs')
- grad_taps: float32 [3, 3072], P(None, 'tp')
- rows_gate: float32 [2048], P('fs')
- rows_up: float32 [2048], P('fs')
- rows_down: float32 [3072], P('tp')
The draws below stay inside these ranges and needn't reach their ends.
All inputs are finite; a program needn't handle non-finite values.
Results may differ from the reference program's by a relative error of at most 0.025.
Values may be sent and summed in bfloat16 or wider, within the bound.
No kernel may reach another device: no remote copies, remote signals or barrier semaphores. Data moves between devices by JAX's collectives and lax.ppermute only.
A program may use at most 64 MiB of HBM per device.

```python
import jax
import jax.numpy as jnp
from jax import lax

D = 2048
FF = 3072
KW = 3
TOK = 512
TOKENS = 8192
N_REP = 16
N_FS = 4
N_TP = 8


def with_spikes(values, rng, source, target, shards_of, factor):
    owner, partner = [(jnp.arange(values.shape[dim]) // (values.shape[dim] // shards_of)).reshape([-1 if axis == dim else 1 for axis in range(values.ndim)]) for dim in (source, target)]
    chosen = jax.random.permutation(rng, shards_of)[partner]
    strong = (owner == chosen) | (owner == (partner + shards_of // 2) % shards_of)
    return jnp.where(strong, factor * values, values)


def levels(key, shape, split, low, high):
    def one(axis_at, blocks):
        draws = jax.random.uniform(jax.random.fold_in(jax.random.fold_in(key, 6), axis_at), (blocks,), jnp.float32, low / len(split), high / len(split))
        return jnp.repeat(jnp.exp(draws), shape[axis_at] // blocks).reshape((-1,) + (1,) * (len(shape) - axis_at - 1))

    level = one(*split[0])
    for cut in split[1:]:
        level = level * one(*cut)
    return level


def bell_draw(stream_key, extent, spread, most, pieces=(), kind=jnp.bfloat16):
    entries = jax.random.normal(stream_key, extent, jnp.float32) * spread
    if len(pieces) > 0:
        entries = levels(stream_key, extent, pieces, -0.22, 0.18) * entries
    return jnp.clip(entries, min=-most, max=most).astype(kind)


def noise_with(stream_key, shape, scale, reach, pieces, heavy, dtype=jnp.bfloat16):
    entries = scale * jax.random.normal(stream_key, shape, jnp.float32)
    if pieces:
        entries = entries * levels(stream_key, shape, pieces, -0.22, 0.18)
    return jnp.clip(with_spikes(entries, jax.random.fold_in(stream_key, 3), *heavy), -reach, reach).astype(dtype)


def setup_inputs(seed: int = 0) -> dict:
    streams_of = jax.random.split(jax.random.key(seed), 7)
    inputs = bell_draw(streams_of[0], (TOKENS, D), 1.0, 6.0, ((0, 16), (1, 4)))
    w_gate = bell_draw(streams_of[1], (D, FF), D ** -0.5, 0.125, ((0, 4), (1, 8)))
    w_up = bell_draw(streams_of[2], (D, FF), D ** -0.5, 0.125, ((0, 4), (1, 8)))
    conv_taps = bell_draw(streams_of[3], (KW, FF), KW ** -0.5, 3.5, ((1, 8),))
    w_down = bell_draw(streams_of[4], (FF, D), FF ** -0.5, 0.109375, ((0, 8), (1, 4)))
    out_grad = noise_with(streams_of[5], (TOKENS, D), 1.0, 6.0, ((0, 16), (1, 4)), (0, 1, 16, 2.0))
    return {"inputs": inputs, "w_gate": w_gate, "w_up": w_up, "conv_taps": conv_taps, "w_down": w_down, "out_grad": out_grad}


def rounded(values):
    return lax.optimization_barrier(values.astype(jnp.bfloat16)).astype(jnp.float32)


def shift_down(values, lag_rows):
    if lag_rows == 0:
        return values
    padding = jnp.zeros_like(values[:, :lag_rows])
    return jnp.concatenate([padding, values[:, :-lag_rows]], axis=1)


def shift_up(values, lag_rows):
    if lag_rows == 0:
        return values
    padding = jnp.zeros_like(values[:, :lag_rows])
    return jnp.concatenate([values[:, lag_rows:], padding], axis=1)


def contract(left, right, left_dim, right_dim):
    return lax.dot_general(left, right, (((left_dim,), (right_dim,)), ((), ())), preferred_element_type=jnp.float32)


def reference(inputs, w_gate, w_up, conv_taps, w_down, out_grad):
    block_width = D // N_FS
    hidden_block = FF // N_TP
    gate_sum = jnp.zeros((TOKENS, FF), jnp.float32)
    up_sum = jnp.zeros((TOKENS, FF), jnp.float32)
    act_sum = jnp.zeros((TOKENS, FF), jnp.float32)
    for block_id in range(N_FS):
        start_col = block_id * block_width
        end_col = start_col + block_width
        gate_sum = gate_sum + rounded(jnp.dot(inputs[:, start_col:end_col], w_gate[start_col:end_col], preferred_element_type=jnp.float32))
        up_sum = up_sum + rounded(jnp.dot(inputs[:, start_col:end_col], w_up[start_col:end_col], preferred_element_type=jnp.float32))
        act_sum = act_sum + rounded(contract(out_grad[:, start_col:end_col], w_down[:, start_col:end_col], 1, 1))
    gate_pre = gate_sum.astype(jnp.bfloat16)
    up_val = up_sum.astype(jnp.bfloat16)
    act_grad = act_sum.astype(jnp.bfloat16)
    tap_weights = conv_taps.astype(jnp.float32)
    gate_seq = gate_pre.astype(jnp.float32).reshape(N_REP, TOK, FF)
    up_seq = up_val.astype(jnp.float32).reshape(N_REP, TOK, FF)
    act_seq = act_grad.astype(jnp.float32).reshape(N_REP, TOK, FF)
    pre_act = jnp.zeros((N_REP, TOK, FF), jnp.float32)
    for tap_index in range(KW):
        pre_act = pre_act + tap_weights[tap_index] * shift_down(gate_seq, KW - 1 - tap_index)
    sigmoid_pre = jax.nn.sigmoid(pre_act)
    hidden = (pre_act * sigmoid_pre * up_seq).astype(jnp.bfloat16)
    up_grad = (act_seq * pre_act * sigmoid_pre).astype(jnp.bfloat16)
    pre_grad = act_seq * up_seq * sigmoid_pre * (1.0 + pre_act * (1.0 - sigmoid_pre))
    gate_grad = jnp.zeros((N_REP, TOK, FF), jnp.float32)
    tap_list = []
    for tap_index in range(KW):
        gate_grad = gate_grad + tap_weights[tap_index] * shift_up(pre_grad, KW - 1 - tap_index)
        tap_list.append(jnp.sum(shift_down(gate_seq, KW - 1 - tap_index) * pre_grad, axis=(0, 1)))
    grad_taps = jnp.stack(tap_list)
    gate_grad = gate_grad.astype(jnp.bfloat16).reshape(TOKENS, FF)
    up_grad = up_grad.reshape(TOKENS, FF)
    hidden = hidden.reshape(TOKENS, FF)
    input_sum = jnp.zeros((TOKENS, D), jnp.float32)
    for block_id in range(N_TP):
        start_col = block_id * hidden_block
        end_col = start_col + hidden_block
        term = contract(gate_grad[:, start_col:end_col], w_gate[:, start_col:end_col], 1, 1)
        term = term + contract(up_grad[:, start_col:end_col], w_up[:, start_col:end_col], 1, 1)
        input_sum = input_sum + rounded(term)
    in_grad = input_sum.astype(jnp.bfloat16)
    grad_gate = contract(inputs, gate_grad, 0, 0)
    grad_up = contract(inputs, up_grad, 0, 0)
    grad_down = contract(hidden, out_grad, 0, 0)
    rows_gate = jnp.sum(grad_gate * grad_gate, axis=1)
    rows_up = jnp.sum(grad_up * grad_up, axis=1)
    rows_down = jnp.sum(grad_down * grad_down, axis=1)
    return (in_grad, grad_gate, grad_up, grad_down, grad_taps, rows_gate, rows_up, rows_down)
```

```python
import jax
import jax.numpy as jnp
from jax import lax
from jax.sharding import PartitionSpec as P

KW = 3
CHUNK = 64


def shift_down(values, lag_rows):
    if lag_rows == 0:
        return values
    padding = jnp.zeros_like(values[:lag_rows])
    return jnp.concatenate([padding, values[:-lag_rows]], axis=0)


def shift_up(values, lag_rows):
    if lag_rows == 0:
        return values
    padding = jnp.zeros_like(values[:lag_rows])
    return jnp.concatenate([values[lag_rows:], padding], axis=0)


def contract(left, right, left_dim, right_dim):
    return lax.dot_general(
        left, right, (((left_dim,), (right_dim,)), ((), ())), preferred_element_type=jnp.float32
    )


def pieces(array, rows):
    return [array[start : start + rows] for start in range(0, array.shape[0], rows)]


def summed(arrays, axis, extra):
    parts = [pieces(array, CHUNK * 384 // array.shape[1]) for array in arrays]
    flat = [piece for group in parts for piece in group]
    tails = [extra[:1], extra[1:]]
    sums = lax.psum(tuple(flat + tails), axis)
    out = []
    at = 0
    for group in parts:
        out.append(jnp.concatenate(sums[at : at + len(group)], axis=0))
        at += len(group)
    return out, jnp.concatenate(sums[at:])


def split_float(values):
    high = values.astype(jnp.bfloat16)
    low = (values - high.astype(jnp.float32)).astype(jnp.bfloat16)
    return high, low


def shards(inputs, w_gate, w_up, conv_taps, w_down, out_grad):
    tap_weights = conv_taps.astype(jnp.float32)
    gate_part = jnp.dot(inputs, w_gate, preferred_element_type=jnp.float32)
    up_part = jnp.dot(inputs, w_up, preferred_element_type=jnp.float32)
    act_part = contract(out_grad, w_down, 1, 1)
    act_part = act_part.astype(jnp.bfloat16)
    (gate_pre, up_val, act_body), act_last = summed(
        [gate_part.astype(jnp.bfloat16), up_part.astype(jnp.bfloat16), act_part[:-CHUNK]],
        "fs",
        act_part[-CHUNK:].reshape(-1),
    )
    act_grad = jnp.concatenate([act_body, act_last.reshape(CHUNK, -1)], axis=0)
    gate_float = gate_pre.astype(jnp.float32)
    up_float = up_val.astype(jnp.float32)
    act_float = act_grad.astype(jnp.float32)
    shifted = [shift_down(gate_float, KW - 1 - tap_index) for tap_index in range(KW)]
    pre_act = tap_weights[0] * shifted[0]
    for tap_index in range(1, KW):
        pre_act = pre_act + tap_weights[tap_index] * shifted[tap_index]
    sigmoid_pre = jax.nn.sigmoid(pre_act)
    hidden = (pre_act * sigmoid_pre * up_float).astype(jnp.bfloat16)
    up_grad = (act_float * pre_act * sigmoid_pre).astype(jnp.bfloat16)
    pre_grad = act_float * up_float * sigmoid_pre * (1.0 + pre_act * (1.0 - sigmoid_pre))
    gate_acc = tap_weights[0] * shift_up(pre_grad, KW - 1)
    for tap_index in range(1, KW):
        gate_acc = gate_acc + tap_weights[tap_index] * shift_up(pre_grad, KW - 1 - tap_index)
    gate_grad = gate_acc.astype(jnp.bfloat16)
    grad_taps = jnp.stack(
        [jnp.sum(shifted[tap_index] * pre_grad, axis=0) for tap_index in range(KW)]
    )
    grad_gate = contract(inputs, gate_grad, 0, 0).astype(jnp.bfloat16)
    grad_up = contract(inputs, up_grad, 0, 0).astype(jnp.bfloat16)
    grad_down = contract(hidden, out_grad, 0, 0).astype(jnp.bfloat16)
    in_part = (contract(gate_grad, w_gate, 1, 1) + contract(up_grad, w_up, 1, 1)).astype(jnp.bfloat16)
    (grad_gate, grad_up, grad_down), grad_taps = summed(
        [grad_gate, grad_up, grad_down], "rep", grad_taps.astype(jnp.bfloat16).reshape(-1)
    )
    grad_gate = grad_gate.astype(jnp.float32)
    grad_up = grad_up.astype(jnp.float32)
    grad_down = grad_down.astype(jnp.float32)
    grad_taps = grad_taps.astype(jnp.float32).reshape(KW, -1)
    gate_rows = jnp.sum(grad_gate * grad_gate, axis=1)
    up_rows = jnp.sum(grad_up * grad_up, axis=1)
    down_rows = jnp.sum(grad_down * grad_down, axis=1)
    n_tp = lax.axis_size("tp")
    n_fs = lax.axis_size("fs")
    rows = jnp.stack([*split_float(gate_rows), *split_float(up_rows)])
    sent = jnp.concatenate(
        [
            in_part.reshape(n_tp, -1, in_part.shape[1]),
            jnp.broadcast_to(rows, (n_tp, *rows.shape)),
        ],
        axis=1,
    )
    got = lax.all_to_all(sent, "tp", 0, 0).astype(jnp.float32).sum(axis=0)
    n_rows = in_part.shape[0] // n_tp
    in_grad = got[:n_rows].astype(jnp.bfloat16)
    gate_rows = got[n_rows] + got[n_rows + 1]
    up_rows = got[n_rows + 2] + got[n_rows + 3]
    down_rows = lax.all_to_all(
        jnp.broadcast_to(down_rows, (n_fs, *down_rows.shape)), "fs", 0, 0
    ).sum(axis=0)
    return (in_grad, grad_gate, grad_up, grad_down, grad_taps, gate_rows, up_rows, down_rows)


def solution(mesh):
    return jax.shard_map(
        shards,
        mesh=mesh,
        in_specs=(
            P("rep", "fs"),
            P("fs", "tp"),
            P("fs", "tp"),
            P(None, "tp"),
            P("tp", "fs"),
            P("rep", "fs"),
        ),
        out_specs=(
            P(("rep", "tp"), "fs"),
            P("fs", "tp"),
            P("fs", "tp"),
            P("tp", "fs"),
            P(None, "tp"),
            P("fs"),
            P("fs"),
            P("tp"),
        ),
        check_vma=False,
    )
```

```python
import jax
import jax.numpy as jnp
from jax import lax
from jax.experimental import pallas as pl
from jax.experimental.pallas import tpu as pltpu
from jax.sharding import PartitionSpec as P

KW = 3
ROWS = 64
UNITS = 48
PAD = 8
NORM_ROWS = 16
BF16 = jnp.bfloat16
F32 = jnp.float32


def contract(left, right, left_dim, right_dim):
    out = lax.dot_general(
        left, right, (((left_dim,), (right_dim,)), ((), ())), preferred_element_type=F32
    )
    return out.astype(BF16)


def pieces(array, rows):
    return [array[start : start + rows] for start in range(0, array.shape[0], rows)]


def call(kernel, out_shape, *args, scratch=()):
    whole = pl.BlockSpec(memory_space=pltpu.VMEM)
    return pl.pallas_call(
        kernel,
        out_shape=out_shape,
        in_specs=[whole] * len(args),
        out_specs=jax.tree.map(lambda _: whole, out_shape),
        scratch_shapes=list(scratch),
        compiler_params=pltpu.CompilerParams(vmem_limit_bytes=32 << 20),
    )(*args)


def corner(shape):
    row = lax.broadcasted_iota(jnp.int32, shape, 0)
    col = lax.broadcasted_iota(jnp.int32, shape, 1)
    return (row == 0) & (col == 0)


def pointwise_kernel(count, *refs):
    gate, up, act = refs[:count], refs[count : 2 * count], refs[2 * count : 3 * count]
    first, taps_in = refs[3 * count : 3 * count + 2]
    gate_grad, up_grad, hidden, taps_out, taps_first = refs[3 * count + 2 : 3 * count + 7]
    gate_pad, pre_pad = refs[3 * count + 7 :]
    width = taps_in.shape[1]
    taps = taps_in[...].astype(F32)
    tap = [taps[j : j + 1] for j in range(KW)]
    gate_pad[:PAD] = jnp.zeros((PAD, width), F32)
    for i in range(count):
        value = gate[i][...].astype(F32)
        if i == 0:
            value = jnp.where(corner(value.shape), first[0:1, 0:1].astype(F32), value)
        gate_pad[PAD + ROWS * i : PAD + ROWS * (i + 1)] = value
    sums = [jnp.zeros((1, width), F32) for _ in range(KW)]
    for i in range(count):
        base = PAD + ROWS * i - (KW - 1)
        shifted = [gate_pad[base + j : base + j + ROWS] for j in range(KW)]
        pre = tap[0] * shifted[0] + tap[1] * shifted[1] + tap[2] * shifted[2]
        sig = jax.nn.sigmoid(pre)
        silu = pre * sig
        up_value = up[i][...].astype(F32)
        act_value = act[i][...].astype(F32)
        rows = slice(ROWS * i, ROWS * (i + 1))
        hidden[rows] = (silu * up_value).astype(BF16)
        up_grad[rows] = (act_value * silu).astype(BF16)
        pre_grad = act_value * up_value * sig * (1.0 + pre * (1.0 - sig))
        pre_pad[rows] = pre_grad
        sums = [
            total + jnp.sum(value * pre_grad, axis=0, keepdims=True)
            for total, value in zip(sums, shifted)
        ]
    pre_pad[ROWS * count :] = jnp.zeros((PAD, width), F32)
    for i in range(count):
        base = ROWS * i
        later = [pre_pad[base + j : base + j + ROWS] for j in range(KW)]
        grad = tap[2] * later[0] + tap[1] * later[1] + tap[0] * later[2]
        gate_grad[base : base + ROWS] = grad.astype(BF16)
    taps_out[...] = jnp.concatenate(sums, axis=0).astype(BF16)
    taps_first[...] = sums[0][0:1, 0:1].astype(BF16)


def norms_kernel(count, *refs):
    gate, up, down = refs[:count], refs[count : 2 * count], refs[2 * count : 3 * count]
    part = refs[3 * count]
    packed, down_out = refs[3 * count + 1 :]
    slots, rows, width = part.shape
    packed[:, :rows] = part[...]
    split = []
    for group in (gate, up):
        total = jnp.zeros((1, width), F32)
        for ref in group:
            value = ref[...].astype(F32)
            total = total + jnp.sum(value * value, axis=0, keepdims=True)
        high = total.astype(BF16).astype(F32)
        split += [high, total - high]
    row = lax.broadcasted_iota(jnp.int32, (NORM_ROWS, width), 0)
    block = jnp.zeros((NORM_ROWS, width), F32)
    for i, value in enumerate(split):
        block = jnp.where(row == i, value, block)
    block = block.astype(BF16)
    for slot in range(slots):
        packed[slot, rows:] = block
    ones = jnp.ones((PAD, width), F32)
    square = jnp.concatenate([ref[...] for ref in down], axis=0).astype(F32)
    square = square * square
    down_out[...] = lax.dot_general(
        ones,
        square,
        (((1,), (1,)), ((), ())),
        precision=lax.Precision.HIGHEST,
        preferred_element_type=F32,
    )


def outputs_kernel(count, *refs):
    gate, up, down = refs[:count], refs[count : 2 * count], refs[2 * count : 3 * count]
    taps, first = refs[3 * count : 3 * count + 2]
    gate_out, up_out, down_out, taps_out = refs[3 * count + 2 :]
    for group, out in ((gate, gate_out), (up, up_out)):
        value = jnp.concatenate([ref[...] for ref in group], axis=0).astype(F32)
        out[...] = value.T
    for i, ref in enumerate(down):
        down_out[UNITS * i : UNITS * (i + 1)] = ref[...].astype(F32)
    value = taps[...].astype(F32)
    taps_out[...] = jnp.where(corner(value.shape), first[0:1, 0:1].astype(F32), value)


def reduce_kernel(got, in_grad, gate_rows, up_rows):
    slots, rows, _ = got.shape
    rows -= NORM_ROWS
    total = got[0].astype(F32)
    for slot in range(1, slots):
        total = total + got[slot].astype(F32)
    in_grad[...] = total[:rows].astype(BF16)
    gate_rows[...] = total[rows : rows + 1] + total[rows + 1 : rows + 2]
    up_rows[...] = total[rows + 2 : rows + 3] + total[rows + 3 : rows + 4]


def shards(inputs, w_gate, w_up, conv_taps, w_down, out_grad):
    tokens, width = inputs.shape
    units = w_gate.shape[1]
    n_tp = lax.axis_size("tp")
    shape = jax.ShapeDtypeStruct

    gate_part = contract(inputs, w_gate, 1, 0)
    up_part = contract(inputs, w_up, 1, 0)
    act_part = contract(out_grad, w_down, 1, 1)
    parts = [piece for part in (gate_part, up_part, act_part) for piece in pieces(part, ROWS)]
    parts = lax.psum((*parts, gate_part[:1, :1]), "fs")

    count = tokens // ROWS
    padded = pltpu.VMEM((tokens + PAD, units), F32)
    gate_grad, up_grad, hidden, taps_part, taps_first = call(
        lambda *refs: pointwise_kernel(count, *refs),
        (
            shape((tokens, units), BF16),
            shape((tokens, units), BF16),
            shape((tokens, units), BF16),
            shape((KW, units), BF16),
            shape((1, 1), BF16),
        ),
        *parts,
        conv_taps,
        scratch=(padded, padded),
    )
    grads = [
        contract(gate_grad, inputs, 0, 0),
        contract(up_grad, inputs, 0, 0),
        contract(hidden, out_grad, 0, 0),
    ]
    grads = [piece for grad in grads for piece in pieces(grad, UNITS)]
    *grads, taps_sum, taps_one = lax.psum((*grads, taps_part, taps_first), "rep")

    in_part = lax.dot_general(
        gate_grad, w_gate, (((1,), (1,)), ((), ())), preferred_element_type=F32
    ) + lax.dot_general(up_grad, w_up, (((1,), (1,)), ((), ())), preferred_element_type=F32)
    in_part = in_part.astype(BF16).reshape(n_tp, tokens // n_tp, width)

    count_units = units // UNITS
    packed, down_rows = call(
        lambda *refs: norms_kernel(count_units, *refs),
        (
            shape((n_tp, tokens // n_tp + NORM_ROWS, width), BF16),
            shape((PAD, units), F32),
        ),
        *grads,
        in_part,
    )
    got = lax.all_to_all(packed, "tp", 0, 0)
    down_rows = lax.psum(down_rows[0], "fs")
    grad_gate, grad_up, grad_down, grad_taps = call(
        lambda *refs: outputs_kernel(count_units, *refs),
        (
            shape((width, units), F32),
            shape((width, units), F32),
            shape((units, width), F32),
            shape((KW, units), F32),
        ),
        *grads,
        taps_sum,
        taps_one,
    )
    in_grad, gate_rows, up_rows = call(
        reduce_kernel,
        (
            shape((tokens // n_tp, width), BF16),
            shape((1, width), F32),
            shape((1, width), F32),
        ),
        got,
    )
    return (
        in_grad,
        grad_gate,
        grad_up,
        grad_down,
        grad_taps,
        gate_rows.reshape(width),
        up_rows.reshape(width),
        down_rows,
    )


def solution(mesh):
    return jax.shard_map(
        shards,
        mesh=mesh,
        in_specs=(
            P("rep", "fs"),
            P("fs", "tp"),
            P("fs", "tp"),
            P(None, "tp"),
            P("tp", "fs"),
            P("rep", "fs"),
        ),
        out_specs=(
            P(("rep", "tp"), "fs"),
            P("fs", "tp"),
            P("fs", "tp"),
            P("tp", "fs"),
            P(None, "tp"),
            P("fs"),
            P("fs"),
            P("tp"),
        ),
        check_vma=False,
    )
```

```python
import jax
import jax.numpy as jnp
from jax import lax
from jax.experimental import pallas as pl
from jax.experimental.pallas import tpu as pltpu
from jax.sharding import PartitionSpec as P

KW = 3
ROWS = 64
UNITS = 48
PAD = 8
LANES = 128
STRIP = 32
NORM_ROWS = 16
BF16 = jnp.bfloat16
F32 = jnp.float32


def call(kernel, out_shape, *args, far=(), scratch=()):
    whole = pl.BlockSpec(memory_space=pltpu.VMEM)
    scratch = [*scratch]
    if far:
        scratch += [pltpu.VMEM(array.shape, array.dtype) for array in far]
        scratch += [pltpu.SemaphoreType.DMA((len(far),))]
    args = (*args, *[pltpu.with_memory_space_constraint(array, pltpu.HBM) for array in far])
    return pl.pallas_call(
        kernel,
        out_shape=out_shape,
        in_specs=[whole] * (len(args) - len(far))
        + [pl.BlockSpec(memory_space=pltpu.HBM)] * len(far),
        out_specs=jax.tree.map(lambda _: whole, out_shape),
        scratch_shapes=list(scratch),
        compiler_params=pltpu.CompilerParams(vmem_limit_bytes=32 << 20),
    )(*args)


def fetch(sources, targets, sems):
    copies = [
        pltpu.make_async_copy(source, target, sems.at[k])
        for k, (source, target) in enumerate(zip(sources, targets))
    ]
    for copy in copies:
        copy.start()
    return copies


def corner(shape):
    row = lax.broadcasted_iota(jnp.int32, shape, 0)
    col = lax.broadcasted_iota(jnp.int32, shape, 1)
    return (row == 0) & (col == 0)


def matmul(left, right, left_dim, right_dim):
    return lax.dot_general(
        left, right, (((left_dim,), (right_dim,)), ((), ())), preferred_element_type=F32
    )


def forward_kernel(*refs):
    sources, outs, first = refs[:5], refs[5:-7], refs[-7]
    local, sems = refs[-6:-1], refs[-1]
    count = len(outs) // 3
    inputs, w_gate, w_up, out_grad, w_down = local
    copies = fetch(sources, local, sems)
    for k, ref in enumerate((w_gate, w_up, w_down)):
        copies[k + 1].wait()
        if k == 0:
            copies[0].wait()
        if k == 2:
            copies[4].wait()
            value = matmul(out_grad[...], w_down[...], 1, 1)
        else:
            value = matmul(inputs[...], ref[...], 1, 0)
        for i in range(count):
            outs[k * count + i][...] = value[ROWS * i : ROWS * (i + 1)].astype(BF16)
        if k == 0:
            first[...] = value[0:1, 0:1].astype(BF16)


def backward_kernel(count, *refs):
    gate, up, act = refs[:count], refs[count : 2 * count], refs[2 * count : 3 * count]
    first = refs[3 * count]
    sources = refs[3 * count + 1 : 3 * count + 6]
    gate_pad, pre_pad, gate_grad, up_grad, hidden = refs[-11:-6]
    local, sems = refs[-6:-1], refs[-1]
    taps_in, inputs, out_grad, w_gate, w_up = local
    *grads, taps_out, taps_first, part = refs[3 * count + 6 : -11]
    copies = fetch(sources, local, sems)
    copies[0].wait()
    width = taps_in.shape[1]
    taps = taps_in[...].astype(F32)
    tokens = ROWS * count
    gate_pad[:PAD] = jnp.zeros((PAD, width), F32)
    pre_pad[tokens:] = jnp.zeros((PAD, width), F32)
    for i in range(count):
        gate_pad[PAD + ROWS * i : PAD + ROWS * (i + 1)] = gate[i][...].astype(F32)
    head = gate_pad[PAD : 2 * PAD, :LANES]
    gate_pad[PAD : 2 * PAD, :LANES] = jnp.where(
        corner(head.shape), first[0:1, 0:1].astype(F32), head
    )
    for lane in range(0, width, LANES):
        cols = slice(lane, lane + LANES)
        tap = [jnp.broadcast_to(taps[j : j + 1, cols], (STRIP, LANES)) for j in range(KW)]
        sums = [jnp.zeros((STRIP, LANES), F32) for _ in range(KW)]
        for start in range(0, tokens, STRIP):
            i, inner = divmod(start, ROWS)
            base = PAD + start - (KW - 1)
            shifted = [gate_pad[base + j : base + j + STRIP, cols] for j in range(KW)]
            pre = tap[0] * shifted[0] + tap[1] * shifted[1] + tap[2] * shifted[2]
            sig = jax.nn.sigmoid(pre)
            silu = pre * sig
            up_value = up[i][inner : inner + STRIP, cols].astype(F32)
            act_value = act[i][inner : inner + STRIP, cols].astype(F32)
            rows = slice(start, start + STRIP)
            hidden[rows, cols] = (silu * up_value).astype(BF16)
            up_grad[rows, cols] = (act_value * silu).astype(BF16)
            pre_grad = act_value * up_value * sig * (1.0 + pre * (1.0 - sig))
            pre_pad[rows, cols] = pre_grad
            sums = [total + value * pre_grad for total, value in zip(sums, shifted)]
        for start in range(0, tokens, STRIP):
            later = [pre_pad[start + j : start + j + STRIP, cols] for j in range(KW)]
            grad = tap[2] * later[0] + tap[1] * later[1] + tap[0] * later[2]
            gate_grad[start : start + STRIP, cols] = grad.astype(BF16)
        for j in range(KW):
            row = jnp.sum(sums[j], axis=0, keepdims=True)
            taps_out[j : j + 1, cols] = row.astype(BF16)
            if lane == 0 and j == 0:
                taps_first[...] = row[0:1, 0:1].astype(BF16)
    for copy in copies[1:]:
        copy.wait()
    x = inputs[...]
    for k, (left, right) in enumerate(((gate_grad, x), (up_grad, x), (hidden, out_grad[...]))):
        value = matmul(left[...], right, 0, 0)
        for i in range(width // UNITS):
            piece = value[UNITS * i : UNITS * (i + 1)].astype(BF16)
            grads[k * (width // UNITS) + i][...] = piece
    value = matmul(gate_grad[...], w_gate[...], 1, 1) + matmul(up_grad[...], w_up[...], 1, 1)
    slots, rows, _ = part.shape
    for slot in range(slots):
        part[slot] = value[rows * slot : rows * (slot + 1)].astype(BF16)


def norms_kernel(count, *refs):
    gate, up, down = refs[:count], refs[count : 2 * count], refs[2 * count : 3 * count]
    part = refs[3 * count]
    packed, down_out = refs[3 * count + 1 :]
    slots, rows, width = part.shape
    packed[:, :rows] = part[...]
    split = []
    for group in (gate, up):
        total = jnp.zeros((1, width), F32)
        for ref in group:
            value = ref[...].astype(F32)
            total = total + jnp.sum(value * value, axis=0, keepdims=True)
        high = total.astype(BF16).astype(F32)
        split += [high, total - high]
    row = lax.broadcasted_iota(jnp.int32, (NORM_ROWS, width), 0)
    block = jnp.zeros((NORM_ROWS, width), F32)
    for i, value in enumerate(split):
        block = jnp.where(row == i, value, block)
    block = block.astype(BF16)
    for slot in range(slots):
        packed[slot, rows:] = block
    ones = jnp.ones((PAD, width), F32)
    square = jnp.concatenate([ref[...] for ref in down], axis=0).astype(F32)
    square = square * square
    down_out[...] = lax.dot_general(
        ones,
        square,
        (((1,), (1,)), ((), ())),
        precision=lax.Precision.HIGHEST,
        preferred_element_type=F32,
    )


def outputs_kernel(count, *refs):
    gate, up, down = refs[:count], refs[count : 2 * count], refs[2 * count : 3 * count]
    taps, first = refs[3 * count : 3 * count + 2]
    gate_out, up_out, down_out, taps_out = refs[3 * count + 2 :]
    for group, out in ((gate, gate_out), (up, up_out)):
        value = jnp.concatenate([ref[...] for ref in group], axis=0).astype(F32)
        out[...] = value.T
    for i, ref in enumerate(down):
        down_out[UNITS * i : UNITS * (i + 1)] = ref[...].astype(F32)
    value = taps[...].astype(F32)
    taps_out[...] = jnp.where(corner(value.shape), first[0:1, 0:1].astype(F32), value)


def reduce_kernel(got, in_grad, gate_rows, up_rows):
    slots, rows, _ = got.shape
    rows -= NORM_ROWS
    total = got[0].astype(F32)
    for slot in range(1, slots):
        total = total + got[slot].astype(F32)
    in_grad[...] = total[:rows].astype(BF16)
    gate_rows[...] = total[rows : rows + 1] + total[rows + 1 : rows + 2]
    up_rows[...] = total[rows + 2 : rows + 3] + total[rows + 3 : rows + 4]


def shards(inputs, w_gate, w_up, conv_taps, w_down, out_grad):
    tokens, width = inputs.shape
    units = w_gate.shape[1]
    n_tp = lax.axis_size("tp")
    shape = jax.ShapeDtypeStruct

    count = tokens // ROWS
    count_units = units // UNITS
    one = shape((1, 1), BF16)
    parts = call(
        forward_kernel,
        (*[shape((ROWS, units), BF16)] * (3 * count), one),
        far=(inputs, w_gate, w_up, out_grad, w_down),
    )
    parts = lax.psum(tuple(parts), "fs")
    padded = pltpu.VMEM((tokens + PAD, units), F32)
    rounded = pltpu.VMEM((tokens, units), BF16)
    *grads, in_part = call(
        lambda *refs: backward_kernel(count, *refs),
        (
            *[shape((UNITS, width), BF16)] * (3 * count_units),
            shape((KW, units), BF16),
            one,
            shape((n_tp, tokens // n_tp, width), BF16),
        ),
        *parts,
        far=(conv_taps, inputs, out_grad, w_gate, w_up),
        scratch=(padded, padded, rounded, rounded, rounded),
    )
    *grads, taps_sum, taps_one = lax.psum(tuple(grads), "rep")

    packed, down_rows = call(
        lambda *refs: norms_kernel(count_units, *refs),
        (
            shape((n_tp, tokens // n_tp + NORM_ROWS, width), BF16),
            shape((PAD, units), F32),
        ),
        *grads,
        in_part,
    )
    got = lax.all_to_all(packed, "tp", 0, 0)
    down_rows = lax.psum(down_rows[0], "fs")
    grad_gate, grad_up, grad_down, grad_taps = call(
        lambda *refs: outputs_kernel(count_units, *refs),
        (
            shape((width, units), F32),
            shape((width, units), F32),
            shape((units, width), F32),
            shape((KW, units), F32),
        ),
        *grads,
        taps_sum,
        taps_one,
    )
    in_grad, gate_rows, up_rows = call(
        reduce_kernel,
        (
            shape((tokens // n_tp, width), BF16),
            shape((1, width), F32),
            shape((1, width), F32),
        ),
        got,
    )
    return (
        in_grad,
        grad_gate,
        grad_up,
        grad_down,
        grad_taps,
        gate_rows.reshape(width),
        up_rows.reshape(width),
        down_rows,
    )


def solution(mesh):
    return jax.shard_map(
        shards,
        mesh=mesh,
        in_specs=(
            P("rep", "fs"),
            P("fs", "tp"),
            P("fs", "tp"),
            P(None, "tp"),
            P("tp", "fs"),
            P("rep", "fs"),
        ),
        out_specs=(
            P(("rep", "tp"), "fs"),
            P("fs", "tp"),
            P("fs", "tp"),
            P("tp", "fs"),
            P(None, "tp"),
            P("fs"),
            P("fs"),
            P("tp"),
        ),
        check_vma=False,
    )
```
